256 devices in a mesh: ep: 16 (over y, x), tp: 16 (over z, core).
Axes of the slice: x: 4, y: 4, z: 8, core: 2. Of those that a mesh axis runs over, the one named last changes fastest.
Arguments:
- tokens: bfloat16 [1024, 4096], P('ep'), may hold values from -6 to 6
- norm_gain: float32 [4096], replicated, may hold values from 0.1 to 1.9
- ffn_gain: float32 [4096], replicated, may hold values from 0.1 to 1.9
- w_in: bfloat16 [4096, 2048], P(None, 'tp'), may hold values from -0.09375 to 0.09375
- decay_rate: float32 [8192], P('tp'), may hold values from 0.02 to 2
- frequency: float32 [8192], P('tp'), may hold values from -3.140625 to 3.140625
- log_step: float32 [128], P('tp'), may hold values from -2.3 to 0
- input_real: float32 [16, 8192], P(None, 'tp'), may hold values from -1 to 1
- input_imag: float32 [16, 8192], P(None, 'tp'), may hold values from -1 to 1
- readout_real: float32 [16, 8192], P(None, 'tp'), may hold values from -0.5 to 0.5
- readout_imag: float32 [16, 8192], P(None, 'tp'), may hold values from -0.5 to 0.5
- skip_gain: float32 [2048], P('tp'), may hold values from -4 to 4
- state_real: float32 [1024, 8192], P('ep', 'tp'), may hold values from -6 to 6
- state_imag: float32 [1024, 8192], P('ep', 'tp'), may hold values from -6 to 6
- w_out: bfloat16 [2048, 4096], P('tp'), may hold values from -0.125 to 0.125
- shared_gate: bfloat16 [4096, 1024], P(None, 'tp'), may hold values from -0.09375 to 0.09375
- shared_up: bfloat16 [4096, 1024], P(None, 'tp'), may hold values from -0.09375 to 0.09375
- shared_down: bfloat16 [1024, 4096], P('tp'), may hold values from -0.1875 to 0.1875
- expert_gate: bfloat16 [64, 4096, 1024], P('ep', 'tp'), may hold values from -0.09375 to 0.09375
- expert_up: bfloat16 [64, 4096, 1024], P('ep', 'tp'), may hold values from -0.09375 to 0.09375
- expert_down: bfloat16 [64, 1024, 4096], P('ep', None, 'tp'), may hold values from -0.1875 to 0.1875
- routing: int32 [1024, 4], P('ep'), may hold values from 0 to 63, all different within a row; in each aligned block of 64 rows (0 to 63, 64 to 127, ...) at most 8 rows name the same one
- route_weight: float32 [1024, 4], P('ep'), may hold values from 0.1 to 1
Outputs:
- mixed: bfloat16 [1024, 4096], P('ep', 'tp')
- new_state_real: float32 [1024, 8192], P('ep', 'tp')
- new_state_imag: float32 [1024, 8192], P('ep', 'tp')
The draws below stay inside these ranges and needn't reach their ends.
Inputs may be any that keep to these rules, and one draw needn't show every extreme that they name: `routing`: each row names 4 different experts. In the rows of one index of ep (aligned blocks of 64 rows) no expert is named more than 8 times, and in every draw some expert is named exactly 8 times in some block.
All inputs are finite; a program needn't handle non-finite values.
Results may differ from the reference program's by a relative error of at most 0.02.
Values may be sent and summed in bfloat16 or wider, within the bound.
A program may use at most 64 MiB of HBM per device.

```python
import math
import jax
import jax.numpy as jnp
import numpy as np
from jax import lax

D = 4096
GROUPS = 128
CHAN = 16
STATE = 64
FE = 1024
FS = 1024
TOP_K = 4
SEQ_DEV = 64
SEQS = 1024
EXPERTS = 64
CAP = 8


def steps_of(rng, dims, pieces, low, high):
    loudness, own = 1.0, jax.random.fold_in(rng, 6)
    for axis_at, shards_of in pieces:
        heights = jnp.exp(jax.random.uniform(jax.random.fold_in(own, axis_at), (shards_of,), jnp.float32, low / len(pieces), high / len(pieces)))
        loudness = loudness * jnp.repeat(heights, dims[axis_at] // shards_of).reshape([-1 if axis == axis_at else 1 for axis in range(len(dims))])
    return loudness


def routed_block(key, own, number, rows, amount, top, most, skew):
    sequence = jax.random.permutation(key, amount)
    heavy_load, usual = load_shares(amount, rows * top, most, skew, True), load_shares(amount, rows * top, most, skew, False)
    places = jnp.arange(amount)

    def named(tallies, rotation):
        used = int((tallies > 0).sum())
        fixed = max(1, used // 4)
        shifted = fixed + (places - fixed + rotation * (used - fixed)) % max(1, amount - fixed)
        return jnp.zeros((amount,), jnp.int32).at[sequence[jnp.where(places < fixed, places, shifted)]].set(jnp.asarray(tallies, jnp.int32))

    tallies = jnp.where(number % 4 == 0, named(heavy_load, number // 4), named(usual, number - number // 4 - 1))
    mixed = jax.random.permutation(jax.random.fold_in(own, 3), amount)
    source_of, taker = mixed[0:amount // 2 * 2:2], mixed[1:amount // 2 * 2:2]
    margin = jnp.minimum(tallies[source_of] - 1, most - tallies[taker]) // 2
    margin = jnp.where((source_of == sequence[0]) | (taker == sequence[0]) | (tallies[taker] == 0), 0, jnp.maximum(margin, 0))
    shifted = jax.random.randint(jax.random.fold_in(own, 4), (amount // 2,), 0, 1 << 20) % (margin + 1)
    tallies = tallies.at[source_of].add(-shifted).at[taker].add(shifted)
    members = jnp.searchsorted(jnp.cumsum(tallies), jnp.arange(rows * top), side="right").astype(jnp.int32)
    table = members.reshape(top, rows).T
    table = table[jax.random.permutation(jax.random.fold_in(own, 1), rows)]
    rotation = jax.random.randint(jax.random.fold_in(own, 2), (rows, 1), 0, top)
    return jnp.take_along_axis(table, (jnp.arange(top)[None, :] + rotation) % top, axis=1)


def load_shares(count, total, bound, skew, full):
    loads = [(1 << 20) // math.isqrt(standing ** skew) + 1 for standing in range(1, count + 1)]
    largest = bound if full else min(bound, max(-(-total // count), total * loads[0] // sum(loads)))
    least = 1 if total - largest >= count - 1 else 0
    holding, spare = [largest] + [least] * (count - 1), total - largest - least * (count - 1)
    while spare > 0:
        free = [i for i in range(1, count) if holding[i] < largest] or [i for i in range(1, count) if holding[i] < bound]
        mass, budget = sum([loads[i] for i in free]), spare
        for i in free:
            more = min(bound - holding[i], max(1, budget * loads[i] // mass), spare)
            holding[i] = holding[i] + more
            spare = spare - more
    return np.array(holding)


def noise(own_key, dims, scale, reach, pieces=(), kind=jnp.bfloat16):
    entries = jax.random.normal(own_key, dims, jnp.float32) * scale
    if len(pieces) > 0:
        entries = steps_of(own_key, dims, pieces, -0.22, 0.18) * entries
    return jnp.clip(entries, min=-reach, max=reach).astype(kind)


def setup_inputs(seed: int = 0) -> dict:
    streams_of = jax.random.split(jax.random.key(seed), 24)
    tokens = noise(streams_of[0], (SEQS, D), 1.0, 6.0, ((0, 16),))
    norm_gain = jnp.clip(1.0 + 0.18 * jax.random.normal(streams_of[1], (D,), jnp.float32), 0.1, 1.9)
    ffn_gain = jnp.clip(1.0 + 0.18 * jax.random.normal(streams_of[2], (D,), jnp.float32), 0.1, 1.9)
    w_in = noise(streams_of[3], (D, GROUPS * CHAN), D ** -0.5, 0.09375, ((1, 16),))
    decay_rate = jnp.clip(jnp.exp(math.log(2.0) - 4.6051702 * jax.random.uniform(streams_of[4], (GROUPS * STATE,), jnp.float32) ** steps_of(streams_of[4], (GROUPS * STATE,), ((0, 16),), -0.2, 0.2)), 0.02, 2.0)
    frequency = jnp.clip(jax.random.uniform(streams_of[5], (GROUPS * STATE,), jnp.float32, -3.140625, 3.140625), -3.140625, 3.140625)
    log_step = jnp.clip(-2.3 + 2.3 * jax.random.uniform(streams_of[6], (GROUPS,), jnp.float32) ** steps_of(streams_of[6], (GROUPS,), ((0, 16),), -0.2, 0.2), -2.3, 0.0)
    input_real = noise(streams_of[7], (CHAN, GROUPS * STATE), (2 * CHAN) ** -0.5, 1.0, ((1, 16),), jnp.float32)
    input_imag = noise(streams_of[8], (CHAN, GROUPS * STATE), (2 * CHAN) ** -0.5, 1.0, ((1, 16),), jnp.float32)
    readout_real = noise(streams_of[9], (CHAN, GROUPS * STATE), (2 * STATE) ** -0.5, 0.5, ((1, 16),), jnp.float32)
    readout_imag = noise(streams_of[10], (CHAN, GROUPS * STATE), (2 * STATE) ** -0.5, 0.5, ((1, 16),), jnp.float32)
    skip_gain = noise(streams_of[11], (GROUPS * CHAN,), 1.0, 4.0, ((0, 16),), jnp.float32)
    state_real = noise(streams_of[12], (SEQS, GROUPS * STATE), 1.0, 6.0, ((0, 16), (1, 16)), jnp.float32)
    state_imag = noise(streams_of[13], (SEQS, GROUPS * STATE), 1.0, 6.0, ((0, 16), (1, 16)), jnp.float32)
    w_out = noise(streams_of[14], (GROUPS * CHAN, D), (GROUPS * CHAN) ** -0.5, 0.125, ((0, 16),))
    shared_gate = noise(streams_of[15], (D, FS), D ** -0.5, 0.09375, ((1, 16),))
    shared_up = noise(streams_of[16], (D, FS), D ** -0.5, 0.09375, ((1, 16),))
    shared_down = noise(streams_of[17], (FS, D), FS ** -0.5, 0.1875, ((0, 16),))
    expert_gate = noise(streams_of[18], (EXPERTS, D, FE), D ** -0.5, 0.09375, ((0, 16), (1, 16)))
    expert_up = noise(streams_of[19], (EXPERTS, D, FE), D ** -0.5, 0.09375, ((0, 16), (1, 16)))
    expert_down = noise(streams_of[20], (EXPERTS, FE, D), FE ** -0.5, 0.1875, ((0, 16), (2, 16)))
    routing_keys = jax.random.split(jax.random.fold_in(streams_of[21], 1), SEQS // SEQ_DEV)
    routing_turns = jax.random.permutation(jax.random.fold_in(streams_of[21], 3), SEQS // SEQ_DEV)
    routing = jax.vmap(lambda own, number: routed_block(jax.random.fold_in(streams_of[21], 2), own, number, SEQ_DEV, EXPERTS, TOP_K, CAP, 2))(routing_keys, routing_turns).reshape((SEQS, TOP_K))
    route_weight = jnp.clip(jnp.exp(math.log(1.0) - 2.3025851 * jax.random.uniform(streams_of[22], (SEQS, TOP_K), jnp.float32) ** steps_of(streams_of[22], (SEQS, TOP_K), ((0, 16),), -0.2, 0.2)), 0.1, 1.0)
    return {"tokens": tokens, "norm_gain": norm_gain, "ffn_gain": ffn_gain, "w_in": w_in, "decay_rate": decay_rate, "frequency": frequency, "log_step": log_step, "input_real": input_real, "input_imag": input_imag, "readout_real": readout_real, "readout_imag": readout_imag, "skip_gain": skip_gain, "state_real": state_real, "state_imag": state_imag, "w_out": w_out, "shared_gate": shared_gate, "shared_up": shared_up, "shared_down": shared_down, "expert_gate": expert_gate, "expert_up": expert_up, "expert_down": expert_down, "routing": routing, "route_weight": route_weight}


EPS = 1e-06
ROUTED_SCALE = 2.5
HIGH = lax.Precision.HIGHEST

def rms_scale(values_in, gains):
    values = values_in.astype(jnp.float32)
    factor = lax.rsqrt(lax.optimization_barrier(jnp.mean(values * values, axis=-1, keepdims=True)) + EPS)
    return (values * factor * gains).astype(jnp.bfloat16)

def state_update(normed, w_in, decay_rate, frequency, log_step, input_real, input_imag, readout_real, readout_imag, skip_gain, state_real, state_imag):
    seq_count = normed.shape[0]
    groups = log_step.shape[0]
    chan_count = skip_gain.shape[0] // groups
    state_width = decay_rate.shape[0] // groups
    drive_rows = jnp.dot(normed, w_in, preferred_element_type=jnp.float32).astype(jnp.bfloat16)
    drive_f = drive_rows.astype(jnp.float32).reshape(seq_count, groups, chan_count)
    decays = decay_rate.reshape(groups, state_width)
    omegas = frequency.reshape(groups, state_width)
    step_size = jnp.exp(log_step)[:, None]
    pole_mag = jnp.exp(-decays * step_size)
    pole_angle = omegas * step_size
    pole_re = pole_mag * jnp.cos(pole_angle)
    pole_im = pole_mag * jnp.sin(pole_angle)
    pole_norm = decays * decays + omegas * omegas
    diff_re = pole_re - 1.0
    lift_re = (-decays * diff_re + omegas * pole_im) / pole_norm
    lift_im = (-decays * pole_im - omegas * diff_re) / pole_norm
    in_re = input_real.reshape(chan_count, groups, state_width)
    in_im = input_imag.reshape(chan_count, groups, state_width)
    push_re = jnp.einsum('sgh,hgp->sgp', drive_f, in_re, precision=HIGH)
    push_im = jnp.einsum('sgh,hgp->sgp', drive_f, in_im, precision=HIGH)
    old_re = state_real.reshape(seq_count, groups, state_width)
    old_im = state_imag.reshape(seq_count, groups, state_width)
    new_re = pole_re * old_re - pole_im * old_im + lift_re * push_re - lift_im * push_im
    new_im = pole_re * old_im + pole_im * old_re + lift_re * push_im + lift_im * push_re
    out_re = readout_real.reshape(chan_count, groups, state_width)
    out_im = readout_imag.reshape(chan_count, groups, state_width)
    read_rows = jnp.einsum('sgp,hgp->sgh', new_re, out_re, precision=HIGH) - jnp.einsum('sgp,hgp->sgh', new_im, out_im, precision=HIGH)
    read_rows = read_rows + skip_gain.reshape(groups, chan_count) * drive_f
    activated = jax.nn.gelu(read_rows).reshape(seq_count, groups * chan_count).astype(jnp.bfloat16)
    return (activated, new_re.reshape(seq_count, groups * state_width), new_im.reshape(seq_count, groups * state_width))

def reference(tokens, norm_gain, ffn_gain, w_in, decay_rate, frequency, log_step, input_real, input_imag, readout_real, readout_imag, skip_gain, state_real, state_imag, w_out, shared_gate, shared_up, shared_down, expert_gate, expert_up, expert_down, routing, route_weight):
    normed = rms_scale(tokens, norm_gain)
    activated, new_real, new_imag = state_update(normed, w_in, decay_rate, frequency, log_step, input_real, input_imag, readout_real, readout_imag, skip_gain, state_real, state_imag)
    mixer_terms = jnp.dot(activated, w_out, preferred_element_type=jnp.float32)
    resid = (tokens.astype(jnp.float32) + mixer_terms).astype(jnp.bfloat16)
    ffn_rows = rms_scale(resid, ffn_gain)
    shared_gate_rows = jnp.dot(ffn_rows, shared_gate, preferred_element_type=jnp.float32)
    shared_up_rows = jnp.dot(ffn_rows, shared_up, preferred_element_type=jnp.float32)
    shared_inner = (jax.nn.silu(shared_gate_rows) * shared_up_rows).astype(jnp.bfloat16)
    shared = jnp.dot(shared_inner, shared_down, preferred_element_type=jnp.float32)
    seq_total = tokens.shape[0]
    expert_count = expert_gate.shape[0]
    block_count = seq_total // SEQ_DEV
    per_block = SEQ_DEV * TOP_K
    flat_ids = routing.reshape(-1).astype(jnp.int32)
    one_hot = (flat_ids[:, None] == jnp.arange(expert_count, dtype=jnp.int32)[None, :]).astype(jnp.int32)
    blocked = one_hot.reshape(block_count, per_block, expert_count)
    earlier = (jnp.cumsum(blocked, axis=1) - blocked).reshape(seq_total * TOP_K, expert_count)
    slot_rank = lax.optimization_barrier(jnp.sum(earlier * one_hot, axis=1)).astype(jnp.int32)
    block_ids = (jnp.arange(seq_total * TOP_K, dtype=jnp.int32) // per_block).astype(jnp.int32)
    buffer_rows = block_count * CAP
    column = (block_ids * CAP + slot_rank).astype(jnp.int32)
    token_ids = (jnp.arange(seq_total * TOP_K, dtype=jnp.int32) // TOP_K).astype(jnp.int32)
    table = jnp.full((expert_count, buffer_rows), seq_total, jnp.int32).at[flat_ids, column].set(token_ids)
    padded = jnp.concatenate([ffn_rows, jnp.zeros((1, ffn_rows.shape[1]), jnp.bfloat16)], axis=0)

    def one_expert(args):
        index_rows, gate_w, up_w, down_w = args
        picked = padded[index_rows].astype(jnp.float32)
        gate_rows = jnp.dot(picked, gate_w.astype(jnp.float32), preferred_element_type=jnp.float32)
        up_rows = jnp.dot(picked, up_w.astype(jnp.float32), preferred_element_type=jnp.float32)
        inner_rows = (jax.nn.silu(gate_rows) * up_rows).astype(jnp.bfloat16)
        return jnp.dot(inner_rows.astype(jnp.float32), down_w.astype(jnp.float32), preferred_element_type=jnp.float32)
    outputs = lax.map(one_expert, (table, expert_gate, expert_up, expert_down))
    flat_out = outputs.reshape(expert_count * buffer_rows, outputs.shape[2])
    picked_rows = flat_out[(flat_ids * buffer_rows + column).astype(jnp.int32)].reshape(seq_total, TOP_K, outputs.shape[2])
    weights = route_weight / lax.optimization_barrier(jnp.sum(route_weight, axis=1, keepdims=True)) * ROUTED_SCALE
    routed = lax.optimization_barrier(jnp.sum(weights[:, :, None] * picked_rows, axis=1))
    mixed = (resid.astype(jnp.float32) + shared + routed).astype(jnp.bfloat16)
    return (mixed, new_real, new_imag)
```

```python
import functools
import types

import jax
import jax.numpy as jnp
from jax import lax
from jax.experimental import pallas as pl
from jax.experimental.pallas import tpu as pltpu
from jax.sharding import PartitionSpec as P

EPS = 1e-06
ROUTED_SCALE = 2.5
CAP = 8
MESH = pl.DeviceIdType.MESH
F32 = jnp.float32
BF16 = jnp.bfloat16


def mm(a, b):
    return lax.dot_general(a, b, (((1,), (0,)), ((), ())), preferred_element_type=F32)


def mm_nt(a, b):
    return lax.dot_general(a, b, (((1,), (1,)), ((), ())), preferred_element_type=F32)


def iota(shape, dim):
    return lax.broadcasted_iota(jnp.int32, shape, dim)


def silu(v):
    return v / (1.0 + jnp.exp(-v))


def layer(d, *refs):
    n = types.SimpleNamespace(**dict(zip(d.names, refs)))
    ep, tp = lax.axis_index("ep"), lax.axis_index("tp")
    z, c = lax.div(tp, 2), lax.rem(tp, 2)
    oc = 1 - c
    HS, FD, CD, CR, K = d.HS, d.FD, d.CD, d.CR, d.K

    open_scope = []

    def mark(name=None):
        if open_scope:
            open_scope.pop().__exit__(None, None, None)
        if name:
            open_scope.append(jax.named_scope(name))
            open_scope[-1].__enter__()

    mark("greet")
    barrier = pltpu.get_barrier_semaphore()

    def greet_tp(i, carry):
        pl.semaphore_signal(barrier, inc=1, device_id=(ep, lax.rem(tp + i, d.TP)), device_id_type=MESH)
        return carry

    def greet_ep(i, carry):
        for cc in range(2):
            pl.semaphore_signal(
                barrier, inc=1, device_id=(lax.rem(ep + i, d.EP), z * 2 + cc), device_id_type=MESH
            )
        return carry

    lax.fori_loop(1, d.TP, greet_tp, 0)
    lax.fori_loop(1, d.EP, greet_ep, 0)

    mark("loads")
    loads = {}

    def load(name, src, dst):
        loads[name] = pltpu.make_async_copy(src, dst, n.lsem.at[len(loads)])
        loads[name].start()

    load("tok", n.tokens, n.tok)
    load("ng", n.norm_gain, n.ng)
    load("win", n.w_in, n.win)
    load("ls", n.log_step, n.ls)
    load("dec", n.decay_rate, n.dec)
    load("frq", n.frequency, n.frq)
    load("ir", n.input_real, n.ir)
    load("ii", n.input_imag, n.ii)
    load("rt", n.routing, n.rt)
    load("rw", n.route_weight, n.rw)
    load("sr", n.state_real, n.sr)
    load("si", n.state_imag, n.si)
    load("our", n.readout_real, n.our)
    load("oui", n.readout_imag, n.oui)
    load("sk", n.skip_gain, n.sk)
    load("wout", n.w_out, n.wout)
    load("fg", n.ffn_gain, n.fg)
    load("eg", n.expert_gate.at[pl.ds(c * 2, 2)], n.eg.at[c])
    load("eu", n.expert_up.at[pl.ds(c * 2, 2)], n.eu.at[c])
    load("sg", n.shared_gate, n.sgu.at[pl.ds(c * d.FSD, d.FSD)])
    load("su", n.shared_up, n.sgu.at[pl.ds((2 + c) * d.FSD, d.FSD)])
    load("sd", n.shared_down, n.sd.at[pl.ds(c * d.FSD, d.FSD)])
    load("ed", n.expert_down.at[pl.ds(c * 2, 2)], n.ed.at[c])

    mark("slots")
    loads["rt"].wait()
    loads["rw"].wait()
    which = iota((d.E, d.S), 0)
    raw = n.rw[...]
    share = ROUTED_SCALE * raw / jnp.sum(raw, axis=0, keepdims=True)
    member = jnp.zeros((d.E, d.S), F32)
    weight = jnp.zeros((d.E, d.S), F32)
    for k in range(d.KT):
        hit = n.rt[k : k + 1, :] == which
        member = member + jnp.where(hit, 1.0, 0.0)
        weight = weight + jnp.where(hit, share[k : k + 1, :], 0.0)
    before = jnp.where(iota((d.S, d.S), 0) < iota((d.S, d.S), 1), 1.0, 0.0).astype(BF16)
    rank = mm(member.astype(BF16), before)
    wide = (d.E, CAP, d.S)
    slot = jnp.where(
        (jnp.broadcast_to(rank[:, None, :], wide) == iota(wide, 1).astype(F32))
        & (jnp.broadcast_to(member[:, None, :], wide) > 0.5),
        1.0,
        0.0,
    )
    n.place[...] = slot.reshape(d.E * CAP, d.S).astype(BF16)
    shares = (slot * jnp.broadcast_to(weight[:, None, :], wide)).reshape(d.E * CAP, d.S)
    n.comb[...] = shares.T

    mark("poles")
    for name in ("ls", "dec", "frq", "ir", "ii"):
        loads[name].wait()
    lane = iota((1, d.NS), 1)
    step = jnp.zeros((1, d.NS), F32)
    steps = jnp.exp(n.ls[...])
    for g in range(d.G):
        step = jnp.where(lax.div(lane, d.ST) == g, steps[:, g : g + 1], step)
    decay, omega = n.dec[...], n.frq[...]
    mag = jnp.exp(-decay * step)
    angle = omega * step
    pole_re, pole_im = mag * jnp.cos(angle), mag * jnp.sin(angle)
    norm = decay * decay + omega * omega
    diff = pole_re - 1.0
    lift_re = (-decay * diff + omega * pole_im) / norm
    lift_im = (-decay * pole_im - omega * diff) / norm
    in_re, in_im = n.ir[...], n.ii[...]
    own_group = lax.div(iota((d.CH, d.NS), 0), d.CHAN) == lax.div(iota((d.CH, d.NS), 1), d.ST)

    def spread(x):
        return jnp.where(own_group, jnp.concatenate([x] * d.G, axis=0), 0.0)

    map_re = spread(in_re * lift_re - in_im * lift_im)
    map_im = spread(in_re * lift_im + in_im * lift_re)
    hi_re, hi_im = map_re.astype(BF16), map_im.astype(BF16)
    lo_re = (map_re - hi_re.astype(F32)).astype(BF16)
    lo_im = (map_im - hi_im.astype(F32)).astype(BF16)

    mark("wait_tok")
    for name in ("tok", "ng", "win"):
        loads[name].wait()

    mark("project")
    def project(i, carry):
        squares, total = carry
        cols = pl.ds(pl.multiple_of(i * d.KB, d.KB), d.KB)
        x = n.tok[:, cols].astype(F32)
        squares = squares + jnp.sum(x * x, axis=1, keepdims=True)
        total = total + mm((x * n.ng[:, cols]).astype(BF16), n.win[cols, :])
        return squares, total

    squares, total = lax.fori_loop(
        0, d.D // d.KB, project, (jnp.zeros((d.S, 1), F32), jnp.zeros((d.S, d.CH), F32))
    )
    drive = (total * lax.rsqrt(squares / d.D + EPS)).astype(BF16)

    mark("state")
    for name in ("sr", "si", "our", "oui", "sk"):
        loads[name].wait()
    old_re, old_im = n.sr[...], n.si[...]
    new_re = pole_re * old_re - pole_im * old_im + (mm(drive, hi_re) + mm(drive, lo_re))
    new_im = pole_re * old_im + pole_im * old_re + (mm(drive, hi_im) + mm(drive, lo_im))
    n.nr[...] = new_re
    n.ni[...] = new_im
    save_re = pltpu.make_async_copy(n.nr, n.out_re, n.osem.at[0])
    save_im = pltpu.make_async_copy(n.ni, n.out_im, n.osem.at[1])
    save_re.start()
    save_im.start()
    read = mm_nt(new_re.astype(BF16), spread(n.our[...]).astype(BF16)) - mm_nt(
        new_im.astype(BF16), spread(n.oui[...]).astype(BF16)
    )
    read = read + n.sk[...] * drive.astype(F32)
    act = jax.nn.gelu(read).astype(BF16)
    first = c == 0

    mark("mix_parts")
    loads["wout"].wait()
    for zz in range(d.Z):
        part = mm(act, n.wout[:, zz * CD : (zz + 1) * CD]).astype(BF16)
        for h in range(2):
            n.mix[zz, h] = part[:, h * FD : (h + 1) * FD]

    mark("barrier")
    pl.semaphore_wait(barrier, d.TP - 1 + 2 * (d.EP - 1))

    partner = (ep, z * 2 + oc)

    def chip_at(j):
        away = ((j + 1) // 2) * (1 - 2 * (j % 2))
        return lax.rem(z + K + away + d.Z, d.Z)

    def pair_copy(j):
        zz = chip_at(j)
        if j < d.Z - 1:
            src, dst = n.mix.at[zz, :, pl.ds(oc * HS, HS)], n.pair.at[j]
        else:
            src, dst = n.mix.at[z, oc], n.pair_own
        return pltpu.make_async_remote_copy(
            src, dst, n.gsem.at[0], n.psem.at[j], device_id=partner, device_id_type=MESH
        )

    mark("pair")
    n.mix_recv[pl.ds(z * 2, 2)] = jnp.zeros((2, HS, FD), BF16)
    for j in range(d.Z):
        pair_copy(j).start()
    swaps = {}

    def swap(name, src, dst):
        i = len(swaps)
        swaps[name] = pltpu.make_async_remote_copy(
            src, dst, n.wssem.at[i], n.wrsem.at[i], device_id=partner, device_id_type=MESH
        )
        swaps[name].start()


    def tp_sends(src_at, recv, ssem, rsem):
        def go(zz, cc):
            pltpu.make_async_remote_copy(
                src_at(zz, cc), recv.at[tp], ssem, rsem, device_id=(ep, zz * 2 + cc), device_id_type=MESH
            ).start()

        for j in range(d.Z - 1):
            zz = chip_at(j)
            go(zz, 0)
            go(zz, 1)
        go(z, oc)

    def landed(ref, count, sem):
        view = ref.at[pl.ds(0, count)]
        pltpu.make_async_copy(view, view, sem).wait()

    def total_of(recv):
        halves = []
        for h in range(2):
            acc = recv[h].astype(F32)
            for zz in range(1, d.Z):
                acc = acc + recv[zz * 2 + h].astype(F32)
            halves.append(acc)
        return jnp.concatenate(halves, axis=0)

    hops = {(0, 0): K, (0, 1): K - 1, (1, 0): K - 1, (1, 1): K}
    flows = ((0, 0), (1, 1), (0, 1), (1, 0))
    ahead = (lax.rem(z + 1, d.Z), lax.rem(z + d.Z - 1, d.Z))

    def number(way, h, t):
        return (way * 2 + h) * K + t

    def owner_of(way, away):
        return lax.rem(z + (away if way == 0 else d.Z - away), d.Z)

    def small_ring(value, send, recv, last, ssem, rsem, lsem):
        def copy(way, h, t):
            i = number(way, h, t)
            if t == hops[way, h] - 1:
                dst, sem, core = last.at[way * 2 + c], lsem.at[way * 2 + c], h
            else:
                dst, sem, core = recv.at[i], rsem.at[i], c
            return pltpu.make_async_remote_copy(
                send.at[i], dst, ssem, sem, device_id=(ep, ahead[way] * 2 + core), device_id_type=MESH
            )

        def step(way, h, t):
            i = number(way, h, t)
            total = value(way, hops[way, h] - t, h)
            if t > 0:
                copy(way, h, t - 1).wait_recv()
                total = total + recv[i - 1].astype(F32)
            send[i] = total.astype(BF16)
            copy(way, h, t).start()

        def arrived(way, core):
            pltpu.make_async_remote_copy(
                send.at[0],
                last.at[way * 2 + core],
                ssem,
                lsem.at[way * 2 + core],
                device_id=(ep, ahead[way] * 2 + core),
                device_id_type=MESH,
            ).wait_recv()
            return last[way * 2 + core].astype(F32)

        return step, arrived

    mark("mix_send")
    for j in range(d.Z - 1):
        zz = chip_at(j)
        pair_copy(j).wait_recv()
        for h in range(2):
            both = n.mix[zz, h, pl.ds(c * HS, HS)].astype(F32) + n.pair[j, h].astype(F32)
            n.mix_send[j * 2 + h] = both.astype(BF16)
            pltpu.make_async_remote_copy(
                n.mix_send.at[j * 2 + h],
                n.mix_recv.at[tp],
                n.gsem.at[1],
                n.gsem.at[13],
                device_id=(ep, zz * 2 + h),
                device_id_type=MESH,
            ).start()
    mark("mix_wait")
    loads["fg"].wait()
    mine = pl.ds(pl.multiple_of(tp * FD, FD), FD)
    own_tok = n.tok[:, mine].astype(F32)
    own_gain = n.fg[:, mine]
    pair_copy(d.Z - 1).wait_recv()
    mixer = n.mix[z, c].astype(F32) + n.pair_own[...].astype(F32)
    landed(n.mix_recv, d.TP - 2, n.gsem.at[13])
    mixer = mixer + total_of(n.mix_recv)

    swap("eg", n.expert_gate.at[pl.ds(oc * 2, 2)], n.eg.at[c])
    swap("eu", n.expert_up.at[pl.ds(oc * 2, 2)], n.eu.at[c])
    swap("sg", n.shared_gate, n.sgu.at[pl.ds(c * d.FSD, d.FSD)])
    swap("su", n.shared_up, n.sgu.at[pl.ds((2 + c) * d.FSD, d.FSD)])
    mark("dispatch")
    resid = (own_tok + mixer).astype(BF16)
    n.resid[...] = resid
    resid_f = resid.astype(F32)
    rows = (resid_f * own_gain).astype(BF16)

    n.disp_send[...] = mm(n.place[...], rows).astype(BF16).reshape(2 * d.EP, 2 * CAP, FD)

    def dispatch(ee, cc):
        pltpu.make_async_remote_copy(
            n.disp_send.at[ee * 2 + cc],
            n.xin.at[c * d.EP + ep],
            n.gsem.at[2],
            n.gsem.at[3],
            device_id=(ee, z * 2 + cc),
            device_id_type=MESH,
        ).start()

    def dispatch_body(i, carry):
        ee = lax.rem(ep + i, d.EP)
        dispatch(ee, 0)
        dispatch(ee, 1)
        return carry

    lax.fori_loop(1, d.EP, dispatch_body, 0)
    dispatch(ep, oc)
    n.xin[c * d.EP + ep] = n.disp_send[ep * 2 + c]

    mark("squares_rows")
    per_row = jnp.sum(resid_f * resid_f, axis=1, keepdims=True)
    turned = jnp.where(iota((d.S, 128), 0) == iota((d.S, 128), 1), per_row, 0.0)
    n.ss_send[...] = jnp.sum(turned, axis=0, keepdims=True)
    n.ss_recv[tp] = n.ss_send[...]
    tp_sends(lambda zz, cc: n.ss_send, n.ss_recv, n.gsem.at[4], n.gsem.at[5])
    n.rows_send[...] = rows.reshape(2, HS, FD)
    n.rows_recv[tp] = n.rows_send[c]
    tp_sends(lambda zz, cc: n.rows_send.at[cc], n.rows_recv, n.gsem.at[6], n.gsem.at[7])

    swap("sd", n.shared_down, n.sd.at[pl.ds(c * d.FSD, d.FSD)])
    swap("ed", n.expert_down.at[pl.ds(oc * 2, 2)], n.ed.at[c])

    mark("ss_wait")
    landed(n.ss_recv, d.TP - 1, n.gsem.at[5])
    square = n.ss_recv[0]
    for i in range(1, d.TP):
        square = square + n.ss_recv[i]
    factor = lax.rsqrt(square / d.D + EPS)
    row8 = iota((8, 128), 0)
    piece1 = factor.astype(BF16).astype(F32)
    piece2 = (factor - piece1).astype(BF16).astype(F32)
    piece3 = factor - piece1 - piece2
    pieces = jnp.where(row8 == 0, piece1, jnp.where(row8 == 1, piece2, jnp.where(row8 == 2, piece3, 0.0)))
    spread_fac = mm_nt(pieces.astype(BF16)[:, : d.S], n.place[...])
    n.fac_send[...] = jnp.sum(spread_fac, axis=0, keepdims=True)
    n.fac_recv[ep] = n.fac_send[...]

    def fac_body(i, carry):
        pltpu.make_async_remote_copy(
            n.fac_send,
            n.fac_recv.at[ep],
            n.gsem.at[8],
            n.gsem.at[9],
            device_id=(lax.rem(ep + i, d.EP), tp),
            device_id_type=MESH,
        ).start()
        return carry

    lax.fori_loop(1, d.EP, fac_body, 0)

    mark("factors")
    for name in ("eg", "eu"):
        loads[name].wait()
        swaps[name].wait_recv()
    mark("disp_wait")
    landed(n.xin, 2 * d.EP - 1, n.gsem.at[3])
    mark("gate_up")
    half_row = lax.div(lax.rem(iota((d.EP * 2 * CAP, FD), 0), 2 * CAP), CAP)
    for f in range(2):
        x = n.xin[f * d.EP : (f + 1) * d.EP].reshape(d.EP * 2 * CAP, FD).astype(F32)
        for e in range(2):
            n.xm[f, e] = jnp.where(half_row == e, x, 0.0).astype(BF16)

    per_half = d.FH // d.NB

    def gate_up(i, carry):
        cols = pl.ds(pl.multiple_of(i * d.NB, d.NB), d.NB)
        h = lax.div(i, per_half)
        at = lax.rem(i, per_half) * d.NB
        for w, base in ((n.eg, 0), (n.eu, d.FH)):
            acc = jnp.zeros((d.EP * 2 * CAP, d.NB), F32)
            for f in range(2):
                for e in range(2):
                    acc = acc + mm(n.xm[f, e], w[f, e, :, cols])
            n.part[h, :, pl.ds(pl.multiple_of(base + at, d.NB), d.NB)] = acc.astype(BF16)
        return carry

    lax.fori_loop(0, d.FE // d.NB, gate_up, 0)

    mark("ring0")
    def owned(o):
        return pl.ds(pl.multiple_of(o * CR, CR), CR)

    def ring_copy(way, h, t):
        i = number(way, h, t)
        away = hops[way, h] - t
        owner = lax.rem(z + (away if way == 0 else d.Z - away), d.Z)
        if t == 0:
            src = n.part.at[h, owned(owner)]
        else:
            src = n.rs_send.at[i]
        return owner, pltpu.make_async_remote_copy(
            src, n.rs_recv.at[i], n.rsssem, n.rsrsem.at[i], device_id=(ep, ahead[way] * 2 + c), device_id_type=MESH
        )

    def ring_step(way, h, t):
        owner, copy = ring_copy(way, h, t)
        if t > 0:
            ring_copy(way, h, t - 1)[1].wait_recv()
            i = number(way, h, t)
            n.rs_send[i] = (n.rs_recv[i - 1].astype(F32) + n.part[h, owned(owner)].astype(F32)).astype(BF16)
        copy.start()

    for way, h in flows:
        ring_step(way, h, 0)
    for way, h in flows:
        ring_step(way, h, 1)

    mark("rows_wait")
    for name in ("sg", "su"):
        loads[name].wait()
        swaps[name].wait_recv()
    landed(n.rows_recv, d.TP - 1, n.gsem.at[7])
    mark("shared")
    all_rows = jnp.concatenate([n.rows_recv[i] for i in range(d.TP)], axis=1)
    both = mm_nt(all_rows, n.sgu[...])
    own_fac = jnp.sum(
        jnp.where(iota((HS, 128), 1) == iota((HS, 128), 0) + c * HS, factor, 0.0), axis=1, keepdims=True
    )
    shared_inner = (silu(both[:, : 2 * d.FSD] * own_fac) * (both[:, 2 * d.FSD :] * own_fac)).astype(BF16)

    mark("shared_down")
    for name in ("sd",):
        loads[name].wait()
        swaps[name].wait_recv()
    for zz in range(d.Z):
        part = mm(shared_inner, n.sd[:, zz * CD : (zz + 1) * CD]).astype(BF16)
        for h in range(2):
            n.sh[zz, h] = part[:, h * FD : (h + 1) * FD]
    sh_pair = pltpu.make_async_remote_copy(
        n.sh.at[z, oc], n.sh_pair, n.assem, n.arsem, device_id=partner, device_id_type=MESH
    )
    sh_pair.start()

    def sh_value(way, away, h):
        return n.sh[owner_of(way, away), h].astype(F32)

    sh_step, sh_arrived = small_ring(
        sh_value, n.sh_send, n.sh_recv, n.sh_last, n.gsem.at[12], n.shsem, n.shlsem
    )

    mark("ring")
    for t in range(2, K):
        for way, h in flows:
            if t < hops[way, h]:
                ring_step(way, h, t)

    mark("sh0")
    for way, h in flows:
        sh_step(way, h, 0)
    mark("fac_wait")
    landed(n.fac_recv, d.EP - 1, n.gsem.at[9])
    slots = 2 * CAP
    at_slot = iota((slots, d.E * CAP), 0) + ep * (2 * slots) + c * slots
    here = iota((slots, d.E * CAP), 1) == at_slot
    column = jnp.concatenate(
        [
            jnp.sum(jnp.where(here, n.fac_recv[z * d.BPO + b], 0.0), axis=1, keepdims=True)
            for b in range(d.BPO)
        ],
        axis=0,
    )
    mark("ring_last")
    own = owned(z)
    for h in range(2):
        acc = n.part[h, own].astype(F32)
        for way in range(2):
            t = hops[way, h] - 1
            ring_copy(way, h, t)[1].wait_recv()
            acc = acc + n.rs_recv[number(way, h, t)].astype(F32)
        acc = acc * column
        n.inner[h, z] = (silu(acc[:, : d.FH]) * acc[:, d.FH :]).astype(BF16)

    mark("pass0")
    def pass_copy(way, h, t):
        i = number(way, h, t)
        owner = lax.rem(z + (d.Z - t if way == 0 else t), d.Z)
        return pltpu.make_async_remote_copy(
            n.inner.at[h, owner],
            n.inner.at[h, owner],
            n.agssem,
            n.agrsem.at[i],
            device_id=(ep, ahead[way] * 2 + c),
            device_id_type=MESH,
        )

    def arrival(way, h, t):
        i = number(way, h, t)
        owner = lax.rem(z + (d.Z - t - 1 if way == 0 else t + 1), d.Z)
        pltpu.make_async_remote_copy(
            n.inner.at[h, owner],
            n.inner.at[h, owner],
            n.agssem,
            n.agrsem.at[i],
            device_id=(ep, ahead[way] * 2 + c),
            device_id_type=MESH,
        ).wait_recv()

    def down(*owners):
        rows = CR * len(owners)
        odd = lax.div(lax.rem(iota((rows, d.FH), 0), 2 * CAP), CAP)
        accs = [jnp.zeros((rows, FD), F32), jnp.zeros((rows, FD), F32)]
        for h in range(2):
            x = jnp.concatenate([n.inner[h, o].astype(F32) for o in owners], axis=0)
            for e in range(2):
                xe = jnp.where(odd == e, x, 0.0).astype(BF16)
                for f in range(2):
                    accs[f] = accs[f] + mm(xe, n.ed[f, e, h * d.FH : (h + 1) * d.FH, :])
        blocks = [o * d.BPO + b for o in owners for b in range(d.BPO)]
        for i, ee in enumerate(blocks):
            for f in range(2):
                n.ret_send[ee * 2 + f] = accs[f][i * 2 * CAP : (i + 1) * 2 * CAP].astype(BF16)
        for ee in blocks:
            for f in range(2):
                give_back(ee, f)

    def give_back(ee, f):
        is_me = (ee == ep) & (c == f)

        @pl.when(is_me)
        def _():
            n.ret_recv[ep * 2 + c] = n.ret_send[ee * 2 + f]

        @pl.when(jnp.logical_not(is_me))
        def _():
            pltpu.make_async_remote_copy(
                n.ret_send.at[ee * 2 + f],
                n.ret_recv.at[ep * 2 + c],
                n.gsem.at[10],
                n.gsem.at[11],
                device_id=(ee, z * 2 + f),
                device_id_type=MESH,
            ).start()

    for way, h in flows:
        pass_copy(way, h, 0).start()

    mark("sh1")
    for way, h in flows:
        sh_step(way, h, 1)
    mark("down0")
    loads["ed"].wait()
    swaps["ed"].wait_recv()
    down(z)
    for t in range(1, K):
        mark("pass")
        for way, h in flows:
            arrival(way, h, t - 1)
            if t < hops[way, h]:
                pass_copy(way, h, t).start()
        mark("sh_step")
        for way, h in flows:
            if t + 1 < hops[way, h]:
                sh_step(way, h, t + 1)
        mark("down")
        down(lax.rem(z + d.Z - t, d.Z), lax.rem(z + t, d.Z))
    mark("pass_last")
    arrival(0, 0, K - 1)
    arrival(1, 1, K - 1)
    mark("down_last")
    down(lax.rem(z + K, d.Z))
    mark("sh_wait")
    comb = n.comb[...]
    comb_hi = comb.astype(BF16)
    comb_lo = (comb - comb_hi.astype(F32)).astype(BF16)
    base = n.resid[...].astype(F32)
    sh_pair.wait_recv()
    halves = [sh_arrived(0, core) + sh_arrived(1, core) for core in range(2)]
    mine_sh, other_sh = n.sh[z, c].astype(F32), n.sh_pair[...].astype(F32)
    base = base + jnp.concatenate(
        [halves[0] + jnp.where(first, mine_sh, other_sh), halves[1] + jnp.where(first, other_sh, mine_sh)],
        axis=0,
    )
    mark("ret_wait")
    landed(n.ret_recv, 2 * d.EP - 1, n.gsem.at[11])
    mark("join")
    back = n.ret_recv[...].reshape(d.E * CAP, FD)
    n.fin[...] = (base + mm(comb_hi, back) + mm(comb_lo, back)).astype(BF16)
    save = pltpu.make_async_copy(n.fin, n.out_mixed, n.osem.at[2])
    save.start()

    mark("drain")
    sh_pair.wait_send()
    for copy in swaps.values():
        copy.wait_send()
    landed(n.pair, d.Z, n.gsem.at[0])
    landed(n.mix_send, d.TP - 2, n.gsem.at[1])
    landed(n.disp_send, 2 * d.EP - 1, n.gsem.at[2])
    landed(n.ss_recv, d.TP - 1, n.gsem.at[4])
    landed(n.rows_recv, d.TP - 1, n.gsem.at[6])
    landed(n.fac_recv, d.EP - 1, n.gsem.at[8])
    landed(n.ret_send, 2 * d.EP - 1, n.gsem.at[10])
    landed(n.sh_send, 4 * K - 2, n.gsem.at[12])
    landed(n.rs_recv, 4 * K - 2, n.rsssem)
    view = n.agdummy.at[pl.ds(0, 4 * K - 2)]
    pltpu.make_async_copy(view, view, n.agssem).wait()
    save_re.wait()
    save_im.wait()
    save.wait()
    mark()


def hand_out(*refs):
    srcs, dsts, bufs, sem = refs[:3], refs[3:6], refs[6:9], refs[9]
    ins = [pltpu.make_async_copy(s, b, sem.at[i]) for i, (s, b) in enumerate(zip(srcs, bufs))]
    outs = [pltpu.make_async_copy(b, t, sem.at[3 + i]) for i, (b, t) in enumerate(zip(bufs, dsts))]
    for copy in ins:
        copy.start()
    for copy, after in zip(ins, outs):
        copy.wait()
        after.start()
    for copy in outs:
        copy.wait()


ARGS = (
    "tokens",
    "norm_gain",
    "ffn_gain",
    "w_in",
    "decay_rate",
    "frequency",
    "log_step",
    "input_real",
    "input_imag",
    "readout_real",
    "readout_imag",
    "skip_gain",
    "state_real",
    "state_imag",
    "w_out",
    "shared_gate",
    "shared_up",
    "shared_down",
    "expert_gate",
    "expert_up",
    "expert_down",
    "routing",
    "route_weight",
)


def local(d, *args):
    a = dict(zip(ARGS, args))
    for name in ("norm_gain", "ffn_gain", "decay_rate", "frequency", "log_step", "skip_gain"):
        a[name] = a[name].reshape(1, -1)
    for name in ("shared_gate", "shared_up", "routing", "route_weight"):
        a[name] = a[name].T
    d = types.SimpleNamespace(**vars(d))
    d.S, d.D = a["tokens"].shape
    d.HS = d.S // 2
    d.FD = d.D // d.TP
    d.CD = 2 * d.FD
    d.CH = a["w_in"].shape[1]
    d.NS = a["decay_rate"].shape[1]
    d.G = a["log_step"].shape[1]
    d.ST = d.NS // d.G
    d.CHAN = d.CH // d.G
    d.FE = a["expert_gate"].shape[2]
    d.FH = d.FE // 2
    d.NB = min(256, d.FH)
    d.FSD = a["shared_down"].shape[0]
    d.KT = a["routing"].shape[0]
    d.E = d.EP * 4
    d.BPO = d.EP // d.Z
    d.CR = d.BPO * 2 * CAP
    d.K = d.Z // 2
    d.KB = min(512, d.D)
    v = pltpu.VMEM
    dma = pltpu.SemaphoreType.DMA
    ring = 4 * d.K
    scratch = dict(
        tok=v((d.S, d.D), BF16),
        ng=v((1, d.D), F32),
        fg=v((1, d.D), F32),
        win=v((d.D, d.CH), BF16),
        ls=v((1, d.G), F32),
        dec=v((1, d.NS), F32),
        frq=v((1, d.NS), F32),
        ir=v((d.CHAN, d.NS), F32),
        ii=v((d.CHAN, d.NS), F32),
        our=v((d.CHAN, d.NS), F32),
        oui=v((d.CHAN, d.NS), F32),
        sk=v((1, d.CH), F32),
        sr=v((d.S, d.NS), F32),
        si=v((d.S, d.NS), F32),
        nr=v((d.S, d.NS), F32),
        ni=v((d.S, d.NS), F32),
        rt=v((d.KT, d.S), jnp.int32),
        rw=v((d.KT, d.S), F32),
        wout=v((d.CH, d.D), BF16),
        sgu=v((4 * d.FSD, d.D), BF16),
        sd=v((2 * d.FSD, d.D), BF16),
        eg=v((2, 2, d.FD, d.FE), BF16),
        eu=v((2, 2, d.FD, d.FE), BF16),
        ed=v((2, 2, d.FE, d.FD), BF16),
        place=v((d.E * CAP, d.S), BF16),
        comb=v((d.S, d.E * CAP), F32),
        mix=v((d.Z, 2, d.S, d.FD), BF16),
        pair=v((d.Z, 2, d.HS, d.FD), BF16),
        pair_own=v((d.S, d.FD), BF16),
        mix_send=v((d.TP - 2, d.HS, d.FD), BF16),
        mix_recv=v((d.TP, d.HS, d.FD), BF16),
        resid=v((d.S, d.FD), BF16),
        disp_send=v((2 * d.EP, 2 * CAP, d.FD), BF16),
        xin=v((2 * d.EP, 2 * CAP, d.FD), BF16),
        xm=v((2, 2, d.EP * 2 * CAP, d.FD), BF16),
        ss_send=v((1, 128), F32),
        ss_recv=v((d.TP, 1, 128), F32),
        rows_send=v((2, d.HS, d.FD), BF16),
        rows_recv=v((d.TP, d.HS, d.FD), BF16),
        fac_send=v((1, d.E * CAP), F32),
        fac_recv=v((d.EP, 1, d.E * CAP), F32),
        part=v((2, d.EP * 2 * CAP, d.FE), BF16),
        rs_send=v((ring, d.CR, d.FE), BF16),
        rs_recv=v((ring, d.CR, d.FE), BF16),
        inner=v((2, d.Z, d.CR, d.FH), BF16),
        agdummy=v((ring, d.CR, d.FH), BF16),
        ret_send=v((2 * d.EP, 2 * CAP, d.FD), BF16),
        ret_recv=v((2 * d.EP, 2 * CAP, d.FD), BF16),
        sh=v((d.Z, 2, d.HS, d.FD), BF16),
        sh_pair=v((d.HS, d.FD), BF16),
        sh_send=v((ring, d.HS, d.FD), BF16),
        sh_recv=v((ring, d.HS, d.FD), BF16),
        sh_last=v((4, d.HS, d.FD), BF16),
        fin=v((d.S, d.FD), BF16),
        lsem=dma((23,)),
        osem=dma((3,)),
        wssem=dma((6,)),
        wrsem=dma((6,)),
        psem=dma((d.Z,)),
        shsem=dma((ring,)),
        shlsem=dma((4,)),
        assem=dma,
        arsem=dma,
        gsem=dma((14,)),
        rsssem=dma,
        rsrsem=dma((ring,)),
        agssem=dma,
        agrsem=dma((ring,)),
    )
    d.names = tuple(ARGS) + ("out_mixed", "out_re", "out_im") + tuple(scratch)
    anywhere = pl.BlockSpec(memory_space=pl.ANY)
    results = pl.pallas_call(
        functools.partial(layer, d),
        out_shape=(
            jax.ShapeDtypeStruct((d.S, d.FD), BF16),
            jax.ShapeDtypeStruct((d.S, d.NS), F32),
            jax.ShapeDtypeStruct((d.S, d.NS), F32),
        ),
        in_specs=[anywhere] * len(ARGS),
        out_specs=(anywhere,) * 3,
        scratch_shapes=list(scratch.values()),
        compiler_params=pltpu.CompilerParams(
            collective_id=0, has_side_effects=True, vmem_limit_bytes=67043328
        ),
        name="layer",
    )(*[a[name] for name in ARGS])
    return pl.pallas_call(
        hand_out,
        out_shape=tuple(jax.ShapeDtypeStruct(r.shape, r.dtype) for r in results),
        in_specs=[anywhere] * 3,
        out_specs=(anywhere,) * 3,
        scratch_shapes=[v(r.shape, r.dtype) for r in results] + [dma((6,))],
        compiler_params=pltpu.CompilerParams(vmem_limit_bytes=67043328),
        name="hand_out",
    )(*results)


def solution(mesh):
    d = types.SimpleNamespace(EP=mesh.shape["ep"], TP=mesh.shape["tp"], Z=mesh.shape["tp"] // 2)
    placed = (
        P("ep", None),
        P(),
        P(),
        P(None, "tp"),
        P("tp"),
        P("tp"),
        P("tp"),
        P(None, "tp"),
        P(None, "tp"),
        P(None, "tp"),
        P(None, "tp"),
        P("tp"),
        P("ep", "tp"),
        P("ep", "tp"),
        P("tp", None),
        P(None, "tp"),
        P(None, "tp"),
        P("tp", None),
        P("ep", "tp", None),
        P("ep", "tp", None),
        P("ep", None, "tp"),
        P("ep", None),
        P("ep", None),
    )
    return jax.shard_map(
        functools.partial(local, d),
        mesh=mesh,
        in_specs=placed,
        out_specs=(P("ep", "tp"), P("ep", "tp"), P("ep", "tp")),
        check_vma=False,
    )
```
